1024 devices in a mesh: grp: 2 (over x), fs: 16 (over z), tp: 32 (over y, core).
Axes of the slice: x: 2, y: 16, z: 16, core: 2. Of those that a mesh axis runs over, the one named last changes fastest.
The devices are a block of a 4x16x16 slice.
Arguments:
- tokens: bfloat16 [4096, 3584], P(('grp', 'fs')), parts along dimension 0, may hold values from -6 to 6
- norm_gain: float32 [3584], P('fs'), may hold values from 0.1 to 1.9
- up_master: float32 [3584, 14336], P('fs', 'tp'), may hold values from -0.09375 to 0.09375
- down_master: float32 [3584, 14336], P('fs', 'tp'), may hold values from -0.046875 to 0.046875
Outputs:
- up_ready: bfloat16 [7168, 14336], P('grp', 'tp'), parts along dimension 0
- down_ready: bfloat16 [7168, 14336], P('grp', 'tp'), parts along dimension 0
- mixed_out: bfloat16 [4096, 3584], P(('grp', 'fs', 'tp')), parts along dimension 0
The draws below stay inside these ranges and needn't reach their ends.
There are 2 independent parts, one for each index of `grp`. The reference program is written for one: setup_inputs(seed, part) draws one part's arguments, and reference() takes and returns one part's arrays. A program takes and returns all parts, laid end to end along the dimension named above; an argument that names none is the same for every part. Nothing has to cross between parts.
All inputs are finite; a program needn't handle non-finite values.
Results may differ from the reference program's by a relative error of at most 0.024.
Values may be sent and summed in bfloat16 or wider, within the bound.
A program may use at most 64 MiB of HBM per device.

```python
import jax
import jax.numpy as jnp
from jax import lax

D = 3584
FF = 14336
TOKENS = 2048


def steps_of(own_key, shape, pieces, low, top_value):
    loudness = 1.0
    for position, blocks in pieces:
        draws = jax.random.uniform(jax.random.fold_in(jax.random.fold_in(own_key, 6), position), (blocks,), jnp.float32, low / len(pieces), top_value / len(pieces))
        loudness = loudness * jnp.repeat(jnp.exp(draws), shape[position] // blocks).reshape((-1,) + (1,) * (len(shape) - 1 - position))
    return loudness


def noise(rng, shape, scale, most, pieces=(), held_as=jnp.bfloat16):
    loudness = steps_of(rng, shape, pieces, -0.22, 0.18) if pieces else 1.0
    values = jax.random.normal(rng, shape, jnp.float32) * scale * loudness
    return jnp.minimum(jnp.maximum(values, -most), most).astype(held_as)


def setup_inputs(seed: int = 0, part: int = 0) -> dict:
    keys = jax.random.split(jax.random.key(seed), 5)
    part_splits = jax.random.split(jax.random.fold_in(keys[4], part), 5)
    tokens = noise(part_splits[0], (TOKENS, D), 1.0, 6.0, ((0, 16),))
    norm_gain = jnp.clip(1.0 + 0.18 * jax.random.normal(keys[1], (D,), jnp.float32), 0.1, 1.9)
    up_master = noise(keys[2], (D, FF), D ** -0.5, 0.09375, ((0, 16), (1, 32)), jnp.float32)
    down_master = noise(keys[3], (D, FF), FF ** -0.5, 0.046875, ((0, 16), (1, 32)), jnp.float32)
    return dict(tokens=tokens, norm_gain=norm_gain, up_master=up_master, down_master=down_master)


def reference(tokens, norm_gain, up_master, down_master):
    up_ready = (norm_gain[:, None] * up_master).astype(jnp.bfloat16)
    down_ready = down_master.astype(jnp.bfloat16)
    values = tokens.astype(jnp.float32)
    square_mean = lax.optimization_barrier(jnp.mean(values * values, axis=1, keepdims=True))
    normed = (values * lax.rsqrt(square_mean + 1e-06)).astype(jnp.bfloat16)
    up_acts = jnp.dot(normed, up_ready, preferred_element_type=jnp.float32)
    hidden = jnp.square(jax.nn.relu(up_acts)).astype(jnp.bfloat16)
    mixed_out = lax.dot_general(hidden, down_ready, (((1,), (1,)), ((), ())), preferred_element_type=jnp.float32)
    return (up_ready, down_ready, mixed_out.astype(jnp.bfloat16))
```

```python
import functools

import jax
import jax.numpy as jnp
from jax import lax
from jax.experimental import pallas as pl
from jax.experimental.pallas import tpu as pltpu
from jax.sharding import PartitionSpec as P

MESH = pl.DeviceIdType.MESH
LANES = 128
TILE = 16
GROUPS = 4
CORES = 2
BF16, F32 = jnp.bfloat16, jnp.float32


def pack_rows(rows, cols):
    whole = cols // LANES * LANES
    return rows * (whole // LANES) + rows * (cols - whole) // LANES


def pack(value, ref, base):
    rows, cols = value.shape
    whole = cols // LANES
    for k in range(whole):
        ref[pl.ds(base + k * rows, rows), :] = value[:, k * LANES : (k + 1) * LANES]
    if cols % LANES:
        part = rows // GROUPS
        rest = value[:, whole * LANES :]
        side = jnp.concatenate([rest[k * part : (k + 1) * part] for k in range(GROUPS)], axis=1)
        for k in range(side.shape[1] // LANES):
            ref[pl.ds(base + whole * rows + k * part, part), :] = side[:, k * LANES : (k + 1) * LANES]


def unpack(ref, base, rows, cols):
    whole = cols // LANES
    parts = [ref[pl.ds(base + k * rows, rows), :] for k in range(whole)]
    width = cols - whole * LANES
    if width:
        part = rows // GROUPS
        side = jnp.concatenate(
            [ref[pl.ds(base + whole * rows + k * part, part), :] for k in range(GROUPS * width // LANES)], axis=1
        )
        parts.append(jnp.concatenate([side[:, k * width : (k + 1) * width] for k in range(GROUPS)], axis=0))
    return jnp.concatenate(parts, axis=1)


def main_kernel(
    nz, ntp, rows, cols,
    tokens, gain, up_master, down_master,
    up_all, down_all, mixed,
    tok, gain_v, up_f, down_f, normed, acts, hid, own, pair_out, pair_in, msg_out, msg_in, keep,
    load_sem, zsend, zrecv, xsend, xrecv, psend, precv, ysend, yrecv,
):
    g, z, t = lax.axis_index("grp"), lax.axis_index("fs"), lax.axis_index("tp")
    y, c = t // CORES, t % CORES
    ny = ntp // CORES
    role = g % 2
    half_ring = nz // 2
    z_r, z_l = (z + 1) % nz, (z + nz - 1) % nz
    g_x = g + 1 - 2 * role
    t_core = t + 1 - 2 * c
    size = pack_rows(cols, rows)
    tiles = size // TILE
    e_tiles = tiles // 3
    s_tiles = tiles - 2 * e_tiles
    e_rows, s_rows = e_tiles * TILE, s_tiles * TILE
    q = mixed.shape[1]
    n_tok = tok.shape[0]
    gathers = (up_all, down_all)

    loads = [
        pltpu.make_async_copy(src, dst, load_sem.at[k])
        for k, (src, dst) in enumerate(((up_master, up_f), (gain, gain_v), (down_master, down_f), (tokens, tok)))
    ]
    for copy in loads:
        copy.start()

    def peer(k):
        return {"tp": ((y + k) % ny) * CORES + c}

    barrier = pltpu.get_barrier_semaphore()
    greeted = [{"fs": z_r}, {"fs": z_l}, {"grp": g_x}, {"tp": t_core}]
    for who in greeted:
        pl.semaphore_signal(barrier, inc=1, device_id=who, device_id_type=MESH)

    @pl.loop(1, ny)
    def _(k):
        pl.semaphore_signal(barrier, inc=1, device_id=peer(k), device_id_type=MESH)

    my_base = pl.multiple_of(z * size, TILE)
    loads[0].wait()
    loads[1].wait()
    pack((gain_v[...] * up_f[...].T).astype(BF16), up_all, my_base)
    loads[2].wait()
    pack(down_f[...].T.astype(BF16), down_all, my_base)

    pl.semaphore_wait(barrier, len(greeted) + ny - 1)

    def chunks():
        e0 = e_tiles // 2
        s0 = s_tiles // 2
        mine = role * (e_rows + s_rows)
        return (
            (True, 0, mine, e0 * TILE),
            (True, 1, mine + e0 * TILE, (e_tiles - e0) * TILE),
            (False, 2, e_rows, s0 * TILE),
            (False, 3, e_rows + s0 * TILE, (s_tiles - s0) * TILE),
        )

    CH = chunks()
    other_row = (1 - role) * (e_rows + s_rows)

    def crosses(step, d, idx):
        return step < half_ring or (step == half_ring and idx % 2 == d)

    def origin(step, d):
        return (z + nz - step) % nz if d == 0 else (z + step) % nz

    def z_copy(a, step, d, ch):
        at = gathers[a].at[pl.ds(pl.multiple_of(origin(step - 1, d) * size + ch[2], TILE), ch[3]), :]
        return pltpu.make_async_remote_copy(
            at, at, zsend.at[a, d, step - 1, ch[1]], zrecv.at[a, d, step - 1, ch[1]],
            device_id={"fs": z_r if d == 0 else z_l}, device_id_type=MESH,
        )

    def z_arrival(a, step, d, ch):
        at = gathers[a].at[pl.ds(pl.multiple_of(origin(step, d) * size + ch[2], TILE), ch[3]), :]
        return pltpu.make_async_remote_copy(
            at, at, zsend.at[a, d, step - 1, ch[1]], zrecv.at[a, d, step - 1, ch[1]],
            device_id={"fs": z_r if d == 0 else z_l}, device_id_type=MESH,
        )

    def x_copy(a, step, d, ch, row):
        at = gathers[a].at[pl.ds(pl.multiple_of(origin(step, d) * size + row, TILE), ch[3]), :]
        return pltpu.make_async_remote_copy(
            at, at, xsend.at[a, d, step - 1, ch[1]], xrecv.at[a, d, step - 1, ch[1]],
            device_id={"grp": g_x}, device_id_type=MESH,
        )

    sent = []

    def send_own(a):
        for ch in CH:
            for d in range(2):
                copy = z_copy(a, 1, d, ch)
                copy.start()
                sent.append(copy)

    def receive(a, step):
        for ch in CH:
            for d in range(2):
                if not crosses(step, d, ch[1]):
                    continue
                z_arrival(a, step, d, ch).wait_recv()
                if crosses(step + 1, d, ch[1]):
                    copy = z_copy(a, step + 1, d, ch)
                    copy.start()
                    sent.append(copy)
                if ch[0]:
                    copy = x_copy(a, step, d, ch, ch[2])
                    copy.start()
                    sent.append(copy)

    def wait_x(a, step):
        first = 0
        for ch in CH:
            if not ch[0]:
                continue
            for d in range(2):
                if crosses(step, d, ch[1]):
                    x_copy(a, step, d, ch, other_row + first).wait_recv()
            first += ch[3]

    def slots(step):
        if step == 0:
            return 0, 1
        return 2 * step - 1, (2 if step < half_ring else 1)

    def block_of(step, i):
        return (z + (2 * i - 1) * step + nz) % nz

    def up_compute(step):
        _, count = slots(step)

        @pl.loop(0, count)
        def _(i):
            b = block_of(step, i)
            w = unpack(up_all, pl.multiple_of(b * size, TILE), cols, rows)
            part = lax.dot_general(normed[b], w, (((1,), (1,)), ((), ())), preferred_element_type=F32)
            if step == 0:
                acts[...] = part
            else:
                acts[...] += part

    def down_compute(step):
        first, count = slots(step)

        @pl.loop(0, count)
        def _(i):
            b = block_of(step, i)
            w = unpack(down_all, pl.multiple_of(b * size, TILE), cols, rows)
            part = jnp.dot(hid[...], w, preferred_element_type=F32)
            own[first + i] = part[: n_tok // 2]
            pair_out[first + i] = part[n_tok // 2 :].astype(BF16)

    groups = [(0, 3)] + [(2 * s - 1, 2) for s in range(2, half_ring)] + [(nz - 1, 1)]

    def pair_copy(k):
        first, count = groups[k]
        at = pl.ds(first, count)
        return pltpu.make_async_remote_copy(
            pair_out.at[at], pair_in.at[at], psend.at[k], precv.at[k],
            device_id={"tp": t_core}, device_id_type=MESH,
        )

    def y_copy(gi, k):
        first, count = groups[gi]
        return pltpu.make_async_remote_copy(
            msg_out.at[k - 1, pl.ds(first, count)], msg_in.at[ny - 1 - k, pl.ds(first, count)],
            ysend.at[gi, k - 1], yrecv.at[gi, ny - 1 - k], device_id=peer(k), device_id_type=MESH,
        )

    def send_pair(k):
        copy = pair_copy(k)
        copy.start()
        sent.append(copy)

    def send_y(gi):
        first, count = groups[gi]
        pair_copy(gi).wait_recv()

        @pl.loop(0, count)
        def _(i):
            j = first + i
            total = own[j] + pair_in[j].astype(F32)
            keep[j] = total[:q]
            rounded = total.astype(BF16)
            for k in range(1, ny):
                msg_out[k - 1, j] = rounded[k * q : (k + 1) * q]

        @pl.loop(1, ny)
        def _(k):
            y_copy(gi, k).start()

    def sum_y(gi):
        first, count = groups[gi]

        @pl.loop(1, ny)
        def _(k):
            y_copy(gi, k).wait_recv()

        @pl.loop(0, count)
        def _(i):
            j = first + i
            total = keep[j]
            for k in range(ny - 1):
                total += msg_in[k, j].astype(F32)
            step = (j + 1) // 2
            b = (z + (1 - 2 * (j % 2)) * step + nz) % nz
            mixed[b] = total

    send_own(0)

    loads[3].wait()

    @pl.loop(0, n_tok // TILE)
    def _(r):
        at = pl.ds(pl.multiple_of(r * TILE, TILE), TILE)
        values = tok[at, :].astype(F32)
        mean = jnp.mean(values * values, axis=1, keepdims=True)
        scaled = (values * lax.rsqrt(mean + 1e-06)).astype(BF16)
        for b in range(nz):
            normed[b, at, :] = scaled[:, b * rows : (b + 1) * rows]

    up_compute(0)

    for step in range(1, half_ring + 1):
        receive(0, step)
        if step == half_ring - 1:
            send_own(1)
        if step >= 3:
            wait_x(0, step - 2)
            up_compute(step - 2)

    for step in range(1, half_ring + 1):
        receive(1, step)
        if step <= 2:
            wait_x(0, half_ring - 2 + step)
            up_compute(half_ring - 2 + step)
        if step == 2:
            active = jnp.maximum(acts[...], 0.0)
            hidden = (active * active).astype(BF16)
            to = lax.broadcasted_iota(jnp.int32, (n_tok, n_tok), 0)
            src = lax.broadcasted_iota(jnp.int32, (n_tok, n_tok), 1)
            half_bits = (n_tok // 2).bit_length() - 1
            q_bits = q.bit_length() - 1
            half = lax.shift_right_logical(to, half_bits)
            hop = lax.shift_right_logical(to & (n_tok // 2 - 1), q_bits)
            want = ((hop + y) & (ny - 1)) * (CORES * q) + (half ^ c) * q + (to & (q - 1))
            order = (src == want).astype(F32).astype(BF16)
            hid[...] = jnp.dot(order, hidden, preferred_element_type=F32).astype(BF16)
            down_compute(0)
        if step >= 3:
            wait_x(1, step - 2)
            down_compute(step - 2)
            if step >= 4:
                send_pair(step - 4)
            if step >= 5:
                send_y(step - 5)

    n_groups = len(groups)
    send_pair(half_ring - 3)
    send_y(half_ring - 4)
    wait_x(1, half_ring - 1)
    down_compute(half_ring - 1)
    send_pair(n_groups - 2)
    send_y(n_groups - 3)
    wait_x(1, half_ring)
    down_compute(half_ring)
    send_pair(n_groups - 1)
    send_y(n_groups - 2)
    send_y(n_groups - 1)
    for gi in range(n_groups):
        sum_y(gi)

    for copy in sent:
        copy.wait_send()

    @pl.loop(1, ny)
    def _(k):
        for gi in range(n_groups):
            y_copy(gi, k).wait_send()


def final_kernel(rows, cols, per, up_all, down_all, mixed, up_ready, down_ready, mixed_out):
    size = pack_rows(cols, rows)
    first = pl.program_id(0) * per
    for i in range(per):
        base = pl.multiple_of((first + i) * size, TILE)
        at = pl.ds(i * rows, rows)
        up_ready[:, at] = unpack(up_all, base, cols, rows)
        down_ready[:, at] = unpack(down_all, base, cols, rows)

    @pl.when(pl.program_id(0) == 0)
    def _():
        for b in range(mixed.shape[0]):
            mixed_out[:, b * rows : (b + 1) * rows] = mixed[b].astype(BF16)


def per_device(nz, ntp, tokens, norm_gain, up_master, down_master):
    rows, cols = up_master.shape
    n_tok, d = tokens.shape
    ny = ntp // CORES
    q = n_tok // ntp
    size = pack_rows(cols, rows)
    half_ring = nz // 2
    n_groups = half_ring
    dma = pltpu.SemaphoreType.DMA
    in_vmem = pl.BlockSpec(memory_space=pltpu.VMEM)
    half = n_tok // 2
    up_all, down_all, mixed = pl.pallas_call(
        functools.partial(main_kernel, nz, ntp, rows, cols),
        out_shape=(
            pltpu.VMEM((nz * size, LANES), BF16),
            pltpu.VMEM((nz * size, LANES), BF16),
            pltpu.VMEM((nz, q, rows), F32),
        ),
        in_specs=[pl.BlockSpec(memory_space=pltpu.HBM)] * 4,
        out_specs=(in_vmem, in_vmem, in_vmem),
        scratch_shapes=[
            pltpu.VMEM((n_tok, d), BF16),
            pltpu.VMEM((1, rows), F32),
            pltpu.VMEM((rows, cols), F32),
            pltpu.VMEM((rows, cols), F32),
            pltpu.VMEM((nz, n_tok, rows), BF16),
            pltpu.VMEM((n_tok, cols), F32),
            pltpu.VMEM((n_tok, cols), BF16),
            pltpu.VMEM((nz, half, rows), F32),
            pltpu.VMEM((nz, half, rows), BF16),
            pltpu.VMEM((nz, half, rows), BF16),
            pltpu.VMEM((ny - 1, nz, q, rows), BF16),
            pltpu.VMEM((ny - 1, nz, q, rows), BF16),
            pltpu.VMEM((nz, q, rows), F32),
            dma((4,)),
            dma((2, 2, half_ring, 4)),
            dma((2, 2, half_ring, 4)),
            dma((2, 2, half_ring, 2)),
            dma((2, 2, half_ring, 2)),
            dma((n_groups,)),
            dma((n_groups,)),
            dma((n_groups, ny - 1)),
            dma((n_groups, ny - 1)),
        ],
        compiler_params=pltpu.CompilerParams(
            collective_id=0, has_side_effects=True, vmem_limit_bytes=40 * 1024 * 1024
        ),
        name="gather_and_mix",
    )(*(pltpu.with_memory_space_constraint(v, pltpu.HBM) for v in (tokens, norm_gain.reshape(1, rows), up_master, down_master)))
    per = GROUPS
    up_ready, down_ready, mixed_out = pl.pallas_call(
        functools.partial(final_kernel, rows, cols, per),
        grid=(nz // per,),
        out_shape=(
            pltpu.HBM((cols, d), BF16),
            pltpu.HBM((cols, d), BF16),
            pltpu.HBM((q, d), BF16),
        ),
        in_specs=[in_vmem] * 3,
        out_specs=(
            pl.BlockSpec((cols, per * rows), lambda i: (0, i)),
            pl.BlockSpec((cols, per * rows), lambda i: (0, i)),
            pl.BlockSpec((q, d), lambda i: (0, 0)),
        ),
        compiler_params=pltpu.CompilerParams(vmem_limit_bytes=20 * 1024 * 1024),
        name="write_out",
    )(up_all, down_all, mixed)
    return up_ready.T, down_ready.T, mixed_out


def solution(mesh):
    return jax.shard_map(
        functools.partial(per_device, mesh.shape["fs"], mesh.shape["tp"]),
        mesh=mesh,
        in_specs=(P(("grp", "fs"), None), P("fs"), P("fs", "tp"), P("fs", "tp")),
        out_specs=(P("grp", "tp"), P("grp", "tp"), P(("grp", "fs", "tp"), None)),
        check_vma=False,
    )
```

```python
import functools

import jax
import jax.numpy as jnp
from jax import lax
from jax.experimental import pallas as pl
from jax.experimental.pallas import tpu as pltpu
from jax.sharding import PartitionSpec as P

MESH = pl.DeviceIdType.MESH
LANES = 128
TILE = 16
GROUPS = 4
CORES = 2
BF16, F32 = jnp.bfloat16, jnp.float32


def pack_rows(rows, cols):
    whole = cols // LANES * LANES
    return rows * (whole // LANES) + rows * (cols - whole) // LANES


def pack(value, ref, base):
    rows, cols = value.shape
    whole = cols // LANES
    for k in range(whole):
        ref[pl.ds(base + k * rows, rows), :] = value[:, k * LANES : (k + 1) * LANES]
    if cols % LANES:
        part = rows // GROUPS
        rest = value[:, whole * LANES :]
        side = jnp.concatenate([rest[k * part : (k + 1) * part] for k in range(GROUPS)], axis=1)
        for k in range(side.shape[1] // LANES):
            ref[pl.ds(base + whole * rows + k * part, part), :] = side[:, k * LANES : (k + 1) * LANES]


def unpack(ref, base, rows, cols):
    whole = cols // LANES
    parts = [ref[pl.ds(base + k * rows, rows), :] for k in range(whole)]
    width = cols - whole * LANES
    if width:
        part = rows // GROUPS
        side = jnp.concatenate(
            [ref[pl.ds(base + whole * rows + k * part, part), :] for k in range(GROUPS * width // LANES)], axis=1
        )
        parts.append(jnp.concatenate([side[:, k * width : (k + 1) * width] for k in range(GROUPS)], axis=0))
    return jnp.concatenate(parts, axis=1)


def main_kernel(
    nz, ntp, rows, cols,
    tokens, gain, up_master, down_master,
    up_out, down_out, mixed,
    tok, gain_v, up_f, down_f, up_all, down_all, normed, acts, hid, own, pair_out, pair_in, msg_out, msg_in, keep,
    load_sem, zsend, zrecv, xsend, xrecv, psend, precv, ysend, yrecv, right_in, x_in, core_in, y_in,
):
    g, z, t = lax.axis_index("grp"), lax.axis_index("fs"), lax.axis_index("tp")
    y, c = t // CORES, t % CORES
    ny = ntp // CORES
    role = g % 2
    cut = nz - nz // 3
    last, late = nz - 1, nz - cut
    near = z == 0
    z_r, z_l = {"fs": (z + 1) % nz}, {"fs": (z + nz - 1) % nz}
    g_x = {"grp": g + 1 - 2 * role}
    t_core = {"tp": t + 1 - 2 * c}
    size = pack_rows(cols, rows)
    tiles = size // TILE
    e_half = tiles // 5 + (tiles % 5 > 2)
    e_rows = 2 * e_half * TILE
    s_rows = size - 2 * e_rows
    q = mixed.shape[0]
    n_tok = tok.shape[0]
    half_tok = n_tok // 2
    wide = GROUPS * rows
    gathers = (up_all, down_all)

    loads = [
        pltpu.make_async_copy(src, dst, load_sem.at[k])
        for k, (src, dst) in enumerate(((up_master, up_f), (gain, gain_v), (down_master, down_f), (tokens, tok)))
    ]
    for copy in loads:
        copy.start()

    def peer(k):
        return {"tp": ((y + k) % ny) * CORES + c}

    def signal(sem, who):
        pl.semaphore_signal(sem, inc=1, device_id=who, device_id_type=MESH)

    barrier = pltpu.get_barrier_semaphore()

    @pl.when(z < last)
    def _():
        signal(barrier, z_r)

    @pl.when(z == 0)
    def _():
        signal(barrier, z_l)

    @pl.loop(jnp.where(z > 0, y + 1, 0), jnp.where(z > 0, ny, y))
    def _(k):
        signal(barrier, {"tp": k * CORES + c})

    @pl.when(c == 1)
    def _():
        signal(barrier, t_core)

    @pl.when(role == 1)
    def _():
        signal(barrier, g_x)

    my_base = pl.multiple_of(z * size, TILE)
    loads[0].wait()
    loads[1].wait()
    pack((gain_v[...] * up_f[...].T).astype(BF16), up_all, my_base)

    neighbours = (z > 0).astype(jnp.int32) + (z == last).astype(jnp.int32)
    y_first = jnp.where(z > 0, y, ny - 1 - y)
    greetings = neighbours + y_first + (1 - c) + (1 - role)

    @pl.when(greetings > 0)
    def _():
        pl.semaphore_wait(barrier, greetings)


    @pl.when(z > 0)
    def _():
        signal(right_in, z_l)

    @pl.loop(jnp.where(z > 0, 0, y + 1), jnp.where(z > 0, y, ny))
    def _(k):
        signal(y_in, {"tp": k * CORES + c})

    @pl.when(c == 0)
    def _():
        signal(core_in, t_core)

    @pl.when(role == 0)
    def _():
        signal(x_in, g_x)

    mine, theirs = role * (e_rows + s_rows), (1 - role) * (e_rows + s_rows)
    step = e_half * TILE
    kinds = ((0, mine, step), (1, mine + step, step), (2, e_rows, s_rows))

    def part(a, b, row, count):
        return gathers[a].at[pl.ds(pl.multiple_of(b * size + row, TILE), count), :]

    def z_copy(d, a, b, kind):
        i, row, count = kind
        at = part(a, b, row, count)
        return pltpu.make_async_remote_copy(
            at, at, zsend.at[d, a, b, i], zrecv.at[a, b, i], device_id=z_r if d == 0 else z_l, device_id_type=MESH
        )

    def x_copy(a, b, i, row):
        at = part(a, b, row + i * step, step)
        return pltpu.make_async_remote_copy(
            at, at, xsend.at[a, b, i], xrecv.at[a, b, i], device_id=g_x, device_id_type=MESH
        )

    def goes_right(b):
        straight = (z >= b) & ((z < last) | (b >= cut))
        return straight | ((z < b) & (b >= cut) & (z < cut - 1))

    def goes_left(b):
        return jnp.where(b < cut, z >= 1, z >= cut + 1)

    def own_sends(d, a):
        for kind in kinds:
            z_copy(d, a, z, kind).start()

    def receive(a, b, d, onward):
        for kind in kinds:
            z_copy(d, a, b, kind).wait_recv()

            @pl.when(onward)
            def _():
                z_copy(d, a, b, kind).start()

            if kind[0] < 2:
                x_copy(a, b, kind[0], mine).start()

    def wait_x(a, b):
        @pl.when(b != z)
        def _():
            for i in range(2):
                x_copy(a, b, i, theirs).wait_recv()

    def add_up(b):
        wait_x(0, b)
        w = unpack(up_all, pl.multiple_of(b * size, TILE), cols, rows)
        acts[...] += lax.dot_general(normed[b], w, (((1,), (1,)), ((), ())), preferred_element_type=F32)

    @pl.when(goes_left(z))
    def _():
        own_sends(1, 0)

    @pl.when(z == last)
    def _():
        own_sends(0, 0)

    loads[2].wait()
    pack(down_f[...].T.astype(BF16), down_all, my_base)

    loads[3].wait()

    @pl.loop(0, n_tok // TILE)
    def _(r):
        at = pl.ds(pl.multiple_of(r * TILE, TILE), TILE)
        values = tok[at, :].astype(F32)
        mean = jnp.mean(values * values, axis=1, keepdims=True)
        scaled = (values * lax.rsqrt(mean + 1e-06)).astype(BF16)
        for b in range(nz):
            normed[b, at, :] = scaled[:, b * rows : (b + 1) * rows]

    @pl.when(goes_left(z))
    def _():
        own_sends(1, 1)

    @pl.when(z < last)
    def _():
        pl.semaphore_wait(right_in, 1)
        own_sends(0, 0)

    @pl.when(z < cut)
    def _():
        own_sends(0, 1)

    acts[...] = jnp.zeros_like(acts)
    add_up(z)

    @pl.when(role == 1)
    def _():
        pl.semaphore_wait(x_in, 1)

    def from_left(a, s):
        b = (z + nz - 1 - s) % nz
        receive(a, b, 0, goes_right(b))

    before = jnp.where(z < cut, 0, z - cut)

    @pl.loop(0, before)
    def _(s):
        from_left(0, s)

    @pl.when(z >= cut)
    def _():
        own_sends(0, 1)

    @pl.loop(0, before)
    def _(s):
        from_left(1, s)

    above = jnp.where(z < cut, cut - 1 - z, last - z)
    lag = GROUPS

    @pl.loop(0, above)
    def _(s):
        turn = s - (above - 2)

        @pl.when(near & (turn >= 0))
        def _():
            @pl.loop(turn, jnp.minimum(2 * turn + 1, late))
            def _(i):
                from_left(0, i)

        for a in range(2):
            receive(a, z + 1 + s, 1, goes_left(z + 1 + s))

        @pl.when((z < cut) & (s >= lag) & (s - lag < z))
        def _():
            for a in range(2):
                from_left(a, s - lag)

        @pl.when(s >= lag)
        def _():
            add_up(z + 1 + s - lag)

    @pl.loop(jnp.where(z < cut, jnp.minimum(z, jnp.maximum(above - lag, 0)), before), z)
    def _(s):
        for a in range(2):
            from_left(a, s)

    @pl.when(z < cut)
    def _():
        @pl.loop(jnp.where(near, min(3, late), 0), late)
        def _(s):
            from_left(0, z + s)

    done = jnp.maximum(above - lag, 0)

    @pl.loop(done, last)
    def _(s):
        b = jnp.where(s < above, z + 1 + s, s - above)
        add_up(jnp.where((z < cut) & (s >= cut - 1), last - (s - (cut - 1)), b))

    active = jnp.maximum(acts[...], 0.0)
    hidden = (active * active).astype(BF16)
    to = lax.broadcasted_iota(jnp.int32, (n_tok, n_tok), 0)
    src = lax.broadcasted_iota(jnp.int32, (n_tok, n_tok), 1)
    half_bits = half_tok.bit_length() - 1
    q_bits = q.bit_length() - 1
    half = lax.shift_right_logical(to, half_bits)
    hop = lax.shift_right_logical(to & (half_tok - 1), q_bits)
    want = ((hop + y) & (ny - 1)) * (CORES * q) + (half ^ c) * q + (to & (q - 1))
    order = (src == want).astype(F32).astype(BF16)
    hid[...] = jnp.dot(order, hidden, preferred_element_type=F32).astype(BF16)

    n_groups = nz // GROUPS

    def columns(k):
        return pl.ds(k * wide, wide)

    def join(source, out, k):
        for i in range(GROUPS):
            base = (k * GROUPS + i) * size
            out[:, k * wide + i * rows : k * wide + (i + 1) * rows] = unpack(source, base, cols, rows)

    def pair_copy(k):
        return pltpu.make_async_remote_copy(
            pair_out.at[k], pair_in.at[k], psend.at[k], precv.at[k], device_id=t_core, device_id_type=MESH
        )

    def y_copy(k, hops):
        return pltpu.make_async_remote_copy(
            msg_out.at[k, hops - 1], msg_in.at[k, ny - 1 - hops],
            ysend.at[k, hops - 1], yrecv.at[k, ny - 1 - hops], device_id=peer(hops), device_id_type=MESH,
        )

    def mix(k):
        for i in range(GROUPS):
            wait_x(1, k * GROUPS + i)
        join(down_all, down_out, k)
        total = jnp.dot(hid[...], down_out[:, columns(k)], preferred_element_type=F32)
        pair_out[k] = total[half_tok:].astype(BF16)
        own[k] = total[:half_tok]

    def send_y(k):
        pair_copy(k).wait_recv()
        total = own[k] + pair_in[k].astype(F32)
        keep[k] = total[:q]
        rounded = total.astype(BF16)
        for hops in range(1, ny):
            msg_out[k, hops - 1] = rounded[hops * q : (hops + 1) * q]

        @pl.loop(1, ny)
        def _(hops):
            y_copy(k, hops).start()

    def sum_y(k):
        @pl.loop(1, ny)
        def _(hops):
            y_copy(k, hops).wait_recv()

        total = keep[k]
        for i in range(ny - 1):
            total += msg_in[k, i].astype(F32)
        mixed[:, columns(k)] = total.astype(BF16)

    @pl.when(c == 1)
    def _():
        pl.semaphore_wait(core_in, 1)

    early = cut // GROUPS
    turns = list(range(early)) + list(reversed(range(early, n_groups)))
    for i, k in enumerate(turns):
        if i == early:
            send_y(turns[i - 1])

            @pl.when(z < cut)
            def _():
                @pl.loop(0, late)
                def _(s):
                    from_left(1, z + s)

        mix(k)
        pair_copy(k).start()
        if i == 0:
            others = jnp.where(z > 0, ny - 1 - y, y)

            @pl.when(others > 0)
            def _():
                pl.semaphore_wait(y_in, others)
        elif i != early:
            send_y(turns[i - 1])
    join(up_all, up_out, 0)
    send_y(turns[-1])
    for k in range(1, n_groups):
        join(up_all, up_out, k)

    @pl.loop(0, nz)
    def _(b):
        for a in range(2):
            @pl.when(b != z)
            def _():
                for i in range(2):
                    x_copy(a, b, i, mine).wait_send()

            @pl.when(goes_right(b))
            def _():
                for kind in kinds:
                    z_copy(0, a, b, kind).wait_send()

            by_left = (b >= z) & ((b < cut) | (z >= cut))

            @pl.when(by_left & goes_left(b))
            def _():
                for kind in kinds:
                    z_copy(1, a, b, kind).wait_send()

    for i, k in enumerate(turns):
        pair_copy(k).wait_send()
        if i == n_groups - 1:
            for before_k in turns[:-1]:
                @pl.loop(1, ny)
                def _(hops):
                    y_copy(before_k, hops).wait_send()
        sum_y(k)

    @pl.loop(1, ny)
    def _(hops):
        y_copy(turns[-1], hops).wait_send()


def final_kernel(up_v, down_v, mixed_v, up_ready, down_ready, mixed_out, sem):
    copies = []
    rows = up_v.shape[0] // GROUPS
    for a, (src, dst) in enumerate(((up_v, up_ready), (down_v, down_ready))):
        for k in range(GROUPS):
            at = pl.ds(k * rows, rows)
            copies.append(pltpu.make_async_copy(src.at[at], dst.at[at], sem.at[a * GROUPS + k]))
    copies.append(pltpu.make_async_copy(mixed_v, mixed_out, sem.at[2 * GROUPS]))
    for copy in copies:
        copy.start()
    for copy in copies:
        copy.wait()


def per_device(nz, ntp, tokens, norm_gain, up_master, down_master):
    rows, cols = up_master.shape
    n_tok, d = tokens.shape
    ny = ntp // CORES
    q = n_tok // ntp
    size = pack_rows(cols, rows)
    n_groups, wide = nz // GROUPS, GROUPS * rows
    dma, regular = pltpu.SemaphoreType.DMA, pltpu.SemaphoreType.REGULAR
    in_vmem, in_hbm = pl.BlockSpec(memory_space=pltpu.VMEM), pl.BlockSpec(memory_space=pltpu.HBM)
    half = n_tok // 2
    results = pl.pallas_call(
        functools.partial(main_kernel, nz, ntp, rows, cols),
        out_shape=(pltpu.VMEM((cols, d), BF16), pltpu.VMEM((cols, d), BF16), pltpu.VMEM((q, d), BF16)),
        in_specs=[in_hbm] * 4,
        out_specs=(in_vmem, in_vmem, in_vmem),
        scratch_shapes=[
            pltpu.VMEM((n_tok, d), BF16),
            pltpu.VMEM((1, rows), F32),
            pltpu.VMEM((rows, cols), F32),
            pltpu.VMEM((rows, cols), F32),
            pltpu.VMEM((nz * size, LANES), BF16),
            pltpu.VMEM((nz * size, LANES), BF16),
            pltpu.VMEM((nz, n_tok, rows), BF16),
            pltpu.VMEM((n_tok, cols), F32),
            pltpu.VMEM((n_tok, cols), BF16),
            pltpu.VMEM((n_groups, half, wide), F32),
            pltpu.VMEM((n_groups, half, wide), BF16),
            pltpu.VMEM((n_groups, half, wide), BF16),
            pltpu.VMEM((n_groups, ny - 1, q, wide), BF16),
            pltpu.VMEM((n_groups, ny - 1, q, wide), BF16),
            pltpu.VMEM((n_groups, q, wide), F32),
            dma((4,)),
            dma((2, 2, nz, 3)),
            dma((2, nz, 3)),
            dma((2, nz, 2)),
            dma((2, nz, 2)),
            dma((n_groups,)),
            dma((n_groups,)),
            dma((n_groups, ny - 1)),
            dma((n_groups, ny - 1)),
            regular,
            regular,
            regular,
            regular,
        ],
        compiler_params=pltpu.CompilerParams(
            collective_id=0, has_side_effects=True, vmem_limit_bytes=40 * 1024 * 1024
        ),
        name="gather_and_mix",
    )(*(pltpu.with_memory_space_constraint(v, pltpu.HBM) for v in (tokens, norm_gain.reshape(1, rows), up_master, down_master)))
    up_ready, down_ready, mixed_out = pl.pallas_call(
        final_kernel,
        out_shape=(pltpu.HBM((cols, d), BF16), pltpu.HBM((cols, d), BF16), pltpu.HBM((q, d), BF16)),
        in_specs=[in_vmem] * 3,
        out_specs=(in_hbm, in_hbm, in_hbm),
        scratch_shapes=[dma((2 * GROUPS + 1,))],
        compiler_params=pltpu.CompilerParams(vmem_limit_bytes=4 * 1024 * 1024),
        name="write_out",
    )(*results)
    return up_ready.T, down_ready.T, mixed_out


def solution(mesh):
    return jax.shard_map(
        functools.partial(per_device, mesh.shape["fs"], mesh.shape["tp"]),
        mesh=mesh,
        in_specs=(P(("grp", "fs"), None), P("fs"), P("fs", "tp"), P("fs", "tp")),
        out_specs=(P("grp", "tp"), P("grp", "tp"), P(("grp", "fs", "tp"), None)),
        check_vma=False,
    )
```

```python
import functools

import jax
import jax.numpy as jnp
from jax import lax
from jax.experimental import pallas as pl
from jax.experimental.pallas import tpu as pltpu
from jax.sharding import PartitionSpec as P

MESH = pl.DeviceIdType.MESH
LANES = 128
TILE = 16
GROUPS = 4
CORES = 2
BF16, F32 = jnp.bfloat16, jnp.float32


def pack_rows(rows, cols):
    whole = cols // LANES * LANES
    return rows * (whole // LANES) + rows * (cols - whole) // LANES


def pack(value, ref, base):
    rows, cols = value.shape
    whole = cols // LANES
    for k in range(whole):
        ref[pl.ds(base + k * rows, rows), :] = value[:, k * LANES : (k + 1) * LANES]
    if cols % LANES:
        part = rows // GROUPS
        rest = value[:, whole * LANES :]
        side = jnp.concatenate([rest[k * part : (k + 1) * part] for k in range(GROUPS)], axis=1)
        for k in range(side.shape[1] // LANES):
            ref[pl.ds(base + whole * rows + k * part, part), :] = side[:, k * LANES : (k + 1) * LANES]


def unpack(ref, base, rows, cols):
    whole = cols // LANES
    parts = [ref[pl.ds(base + k * rows, rows), :] for k in range(whole)]
    width = cols - whole * LANES
    if width:
        part = rows // GROUPS
        side = jnp.concatenate(
            [ref[pl.ds(base + whole * rows + k * part, part), :] for k in range(GROUPS * width // LANES)], axis=1
        )
        parts.append(jnp.concatenate([side[:, k * width : (k + 1) * width] for k in range(GROUPS)], axis=0))
    return jnp.concatenate(parts, axis=1)


def main_kernel(
    nz, ntp, rows, cols,
    tokens, gain, up_master, down_master,
    up_out, down_out, mixed,
    tok, gain_v, up_f, down_f, up_all, down_all, normed, acts, hid, own, pair_out, pair_in, msg_out, msg_in, keep,
    load_sem, zsend, zsend_own, zrecv, xsend, xrecv, psend, precv, ysend, yrecv, right_in, x_in, core_in, y_in,
):
    g, z, t = lax.axis_index("grp"), lax.axis_index("fs"), lax.axis_index("tp")
    y, c = t // CORES, t % CORES
    ny = ntp // CORES
    role = g % 2
    cuts = (nz - nz // 3, nz - nz // 4)
    last, late = nz - 1, nz // 3
    near = z == 0
    z_r, z_l = {"fs": (z + 1) % nz}, {"fs": (z + nz - 1) % nz}
    g_x = {"grp": g + 1 - 2 * role}
    t_core = {"tp": t + 1 - 2 * c}
    size = pack_rows(cols, rows)
    tiles = size // TILE
    e_half = tiles // 5 + (tiles % 5 > 2)
    e_rows = 2 * e_half * TILE
    s_rows = size - 2 * e_rows
    q = mixed.shape[0]
    n_tok = tok.shape[0]
    half_tok = n_tok // 2
    wide = GROUPS * rows
    gathers = (up_all, down_all)

    loads = [
        pltpu.make_async_copy(src, dst, load_sem.at[k])
        for k, (src, dst) in enumerate(((up_master, up_f), (gain, gain_v), (down_master, down_f), (tokens, tok)))
    ]
    for copy in loads:
        copy.start()

    def peer(k):
        return {"tp": ((y + k) % ny) * CORES + c}

    def signal(sem, who):
        pl.semaphore_signal(sem, inc=1, device_id=who, device_id_type=MESH)

    barrier = pltpu.get_barrier_semaphore()

    @pl.when(z < last)
    def _():
        signal(barrier, z_r)

    @pl.when(z == 0)
    def _():
        signal(barrier, z_l)

    @pl.loop(jnp.where(z > 0, y + 1, 0), jnp.where(z > 0, ny, y))
    def _(k):
        signal(barrier, {"tp": k * CORES + c})

    @pl.when(c == 1)
    def _():
        signal(barrier, t_core)

    @pl.when(role == 1)
    def _():
        signal(barrier, g_x)

    my_base = pl.multiple_of(z * size, TILE)
    loads[0].wait()
    loads[1].wait()
    pack((gain_v[...] * up_f[...].T).astype(BF16), up_all, my_base)

    neighbours = (z > 0).astype(jnp.int32) + (z == last).astype(jnp.int32)
    y_first = jnp.where(z > 0, y, ny - 1 - y)
    greetings = neighbours + y_first + (1 - c) + (1 - role)

    @pl.when(greetings > 0)
    def _():
        pl.semaphore_wait(barrier, greetings)


    @pl.when(z > 0)
    def _():
        signal(right_in, z_l)

    @pl.loop(jnp.where(z > 0, 0, y + 1), jnp.where(z > 0, y, ny))
    def _(k):
        signal(y_in, {"tp": k * CORES + c})

    @pl.when(c == 0)
    def _():
        signal(core_in, t_core)

    @pl.when(role == 0)
    def _():
        signal(x_in, g_x)

    mine, theirs = role * (e_rows + s_rows), (1 - role) * (e_rows + s_rows)
    step = e_half * TILE
    kinds = ((0, mine, step), (1, mine + step, step), (2, e_rows, s_rows))

    def part(a, b, row, count):
        return gathers[a].at[pl.ds(pl.multiple_of(b * size + row, TILE), count), :]

    def z_copy(d, a, b, kind, own_left=False):
        i, row, count = kind
        at = part(a, b, row, count)
        sem = zsend_own.at[a] if own_left else zsend.at[a, b]
        return pltpu.make_async_remote_copy(
            at, at, sem, zrecv.at[a, b, i], device_id=z_r if d == 0 else z_l, device_id_type=MESH
        )

    whole_block = (0, 0, e_rows + s_rows)

    def x_copy(a, b, row, count):
        at = part(a, b, row, count)
        return pltpu.make_async_remote_copy(
            at, at, xsend, xrecv.at[a, b], device_id=g_x, device_id_type=MESH
        )

    def goes_right(a, b):
        cut = cuts[a]
        straight = (z >= b) & ((z < last) | (b >= cut))
        return straight | ((z < b) & (b >= cut) & (z < cut - 1))

    def goes_left(a, b):
        return jnp.where(b < cuts[a], z >= 1, z >= cuts[a] + 1)

    def own_sends(d, a):
        for kind in kinds:
            z_copy(d, a, z, kind, own_left=d == 1).start()

    def receive(a, b, d, onward):
        for kind in kinds:
            z_copy(d, a, b, kind).wait_recv()

            @pl.when(onward)
            def _():
                z_copy(d, a, b, kind).start()

            if kind[0] < 2:
                x_copy(a, b, kind[1], kind[2]).start()

    def wait_x(a, b):
        @pl.when(b != z)
        def _():
            x_copy(a, b, theirs, e_rows).wait_recv()

    def add_up(b):
        wait_x(0, b)
        w = unpack(up_all, pl.multiple_of(b * size, TILE), cols, rows)
        acts[...] += lax.dot_general(normed[b], w, (((1,), (1,)), ((), ())), preferred_element_type=F32)

    @pl.when(goes_left(0, z))
    def _():
        own_sends(1, 0)

    @pl.when(z == last)
    def _():
        own_sends(0, 0)

    loads[2].wait()
    pack(down_f[...].T.astype(BF16), down_all, my_base)

    loads[3].wait()

    @pl.loop(0, n_tok // TILE)
    def _(r):
        at = pl.ds(pl.multiple_of(r * TILE, TILE), TILE)
        values = tok[at, :].astype(F32)
        mean = jnp.mean(values * values, axis=1, keepdims=True)
        scaled = (values * lax.rsqrt(mean + 1e-06)).astype(BF16)
        for b in range(nz):
            normed[b, at, :] = scaled[:, b * rows : (b + 1) * rows]

    @pl.when(goes_left(1, z))
    def _():
        own_sends(1, 1)

    @pl.when(z < last)
    def _():
        pl.semaphore_wait(right_in, 1)
        own_sends(0, 0)

    @pl.when(z < cuts[0])
    def _():
        own_sends(0, 1)

    acts[...] = jnp.zeros_like(acts)
    add_up(z)

    @pl.when(role == 1)
    def _():
        pl.semaphore_wait(x_in, 1)

    def from_left(a, s):
        b = (z + nz - 1 - s) % nz
        receive(a, b, 0, goes_right(a, b))

    before = [jnp.where(z < cut, 0, z - cut) for cut in cuts]

    @pl.loop(0, before[0])
    def _(s):
        from_left(0, s)

    @pl.when(z >= cuts[0])
    def _():
        own_sends(0, 1)

    @pl.loop(0, before[1])
    def _(s):
        from_left(1, s)

    above = [jnp.where(z < cut, cut - 1 - z, last - z) for cut in cuts]
    longest = jnp.maximum(above[0], above[1])
    lag = GROUPS
    taken = jnp.where(z < cuts[0], jnp.minimum(z, jnp.maximum(longest - lag, 0)), before[1])

    @pl.loop(0, longest)
    def _(s):
        turn = s - (above[0] - 2)

        @pl.when(near & (turn >= 0))
        def _():
            first = turn * (turn + 1) // 2

            @pl.loop(jnp.minimum(first, late), jnp.minimum(first + turn + 1, late))
            def _(i):
                from_left(0, i)

        for a in range(2):
            @pl.when(s < above[a])
            def _():
                receive(a, z + 1 + s, 1, goes_left(a, z + 1 + s))

        @pl.when((z < cuts[0]) & (s >= lag) & (s - lag < z))
        def _():
            for a in range(2):
                from_left(a, s - lag)

        @pl.when((s >= lag) & (s - lag < above[0]))
        def _():
            add_up(z + 1 + s - lag)

    @pl.loop(taken, z)
    def _(s):
        for a in range(2):
            @pl.when(s >= (before[0] if a == 0 else 0))
            def _():
                from_left(a, s)

    turns_near = max(cuts) - 1 - (cuts[0] - 3)

    @pl.when(z < cuts[0])
    def _():
        @pl.loop(jnp.where(near, min(turns_near * (turns_near + 1) // 2, late), 0), late)
        def _(s):
            from_left(0, z + s)

    done = jnp.minimum(jnp.maximum(longest - lag, 0), above[0])

    @pl.loop(done, last)
    def _(s):
        b = jnp.where(s < above[0], z + 1 + s, s - above[0])
        add_up(jnp.where((z < cuts[0]) & (s >= cuts[0] - 1), last - (s - (cuts[0] - 1)), b))

    active = jnp.maximum(acts[...], 0.0)
    hidden = (active * active).astype(BF16)
    to = lax.broadcasted_iota(jnp.int32, (n_tok, n_tok), 0)
    src = lax.broadcasted_iota(jnp.int32, (n_tok, n_tok), 1)
    half_bits = half_tok.bit_length() - 1
    q_bits = q.bit_length() - 1
    half = lax.shift_right_logical(to, half_bits)
    hop = lax.shift_right_logical(to & (half_tok - 1), q_bits)
    want = ((hop + y) & (ny - 1)) * (CORES * q) + (half ^ c) * q + (to & (q - 1))
    order = (src == want).astype(F32).astype(BF16)
    hid[...] = jnp.dot(order, hidden, preferred_element_type=F32).astype(BF16)

    n_groups = nz // GROUPS

    def columns(k):
        return pl.ds(k * wide, wide)

    def join(source, out, k):
        for i in range(GROUPS):
            base = (k * GROUPS + i) * size
            out[:, k * wide + i * rows : k * wide + (i + 1) * rows] = unpack(source, base, cols, rows)

    def pair_copy(k):
        return pltpu.make_async_remote_copy(
            pair_out.at[k], pair_in.at[k], psend.at[k], precv.at[k], device_id=t_core, device_id_type=MESH
        )

    def y_copy(k, hops):
        return pltpu.make_async_remote_copy(
            msg_out.at[k, hops - 1], msg_in.at[k, ny - 1 - hops],
            ysend.at[k], yrecv.at[k], device_id=peer(hops), device_id_type=MESH,
        )

    def y_all(k):
        return pltpu.make_async_remote_copy(
            msg_out.at[k], msg_in.at[k], ysend.at[k], yrecv.at[k], device_id=peer(1), device_id_type=MESH
        )

    def mix(k):
        for i in range(GROUPS):
            wait_x(1, k * GROUPS + i)
        join(down_all, down_out, k)
        total = jnp.dot(hid[...], down_out[:, columns(k)], preferred_element_type=F32)
        pair_out[k] = total[half_tok:].astype(BF16)
        own[k] = total[:half_tok]

    def send_y(k):
        pair_copy(k).wait_recv()
        total = own[k] + pair_in[k].astype(F32)
        keep[k] = total[:q]
        rounded = total.astype(BF16)
        for hops in range(1, ny):
            msg_out[k, hops - 1] = rounded[hops * q : (hops + 1) * q]

        @pl.loop(1, ny)
        def _(hops):
            y_copy(k, hops).start()

    def sum_y(k):
        y_all(k).wait_recv()
        total = keep[k]
        for i in range(ny - 1):
            total += msg_in[k, i].astype(F32)
        mixed[:, columns(k)] = total.astype(BF16)

    @pl.when(c == 1)
    def _():
        pl.semaphore_wait(core_in, 1)

    late_down = nz - cuts[1]

    def late_from_left(first, end):
        @pl.when(z < cuts[1])
        def _():
            @pl.loop(first, end)
            def _(s):
                from_left(1, z + s)

    early = cuts[1] // GROUPS
    turns = list(range(early)) + list(reversed(range(early, n_groups)))
    late_from_left(0, 1)
    for i, k in enumerate(turns):
        if i == early:
            send_y(turns[i - 1])
            late_from_left(min(early, late_down), late_down)
        mix(k)
        pair_copy(k).start()
        if i == 0:
            others = jnp.where(z > 0, ny - 1 - y, y)

            @pl.when(others > 0)
            def _():
                pl.semaphore_wait(y_in, others)
        elif i != early:
            send_y(turns[i - 1])
        if 0 < i < min(early, late_down):
            late_from_left(i, i + 1)
    join(up_all, up_out, 0)
    send_y(turns[-1])
    for k in range(1, n_groups):
        join(up_all, up_out, k)

    at = up_all.at[pl.ds(0, (nz - 1) * 2 * e_rows), :]
    pltpu.make_async_remote_copy(at, at, xsend, xrecv.at[0, 0], device_id=g_x, device_id_type=MESH).wait_send()

    for a in range(2):
        @pl.when(goes_left(a, z))
        def _():
            z_copy(1, a, z, whole_block, own_left=True).wait_send()

    @pl.loop(0, nz)
    def _(b):
        for a in range(2):
            by_left = (b > z) & ((b < cuts[a]) | (z >= cuts[a]))

            @pl.when(goes_right(a, b) | (by_left & goes_left(a, b)))
            def _():
                z_copy(0, a, b, whole_block).wait_send()

    for i, k in enumerate(turns):
        pair_copy(k).wait_send()
        if i == n_groups - 1:
            for before_k in turns[:-1]:
                y_all(before_k).wait_send()
        sum_y(k)
    y_all(turns[-1]).wait_send()


def final_kernel(up_v, down_v, mixed_v, up_ready, down_ready, mixed_out, sem):
    copies = []
    rows = up_v.shape[0] // GROUPS
    for a, (src, dst) in enumerate(((up_v, up_ready), (down_v, down_ready))):
        for k in range(GROUPS):
            at = pl.ds(k * rows, rows)
            copies.append(pltpu.make_async_copy(src.at[at], dst.at[at], sem.at[a * GROUPS + k]))
    copies.append(pltpu.make_async_copy(mixed_v, mixed_out, sem.at[2 * GROUPS]))
    for copy in copies:
        copy.start()
    for copy in copies:
        copy.wait()


def per_device(nz, ntp, tokens, norm_gain, up_master, down_master):
    rows, cols = up_master.shape
    n_tok, d = tokens.shape
    ny = ntp // CORES
    q = n_tok // ntp
    size = pack_rows(cols, rows)
    n_groups, wide = nz // GROUPS, GROUPS * rows
    dma, regular = pltpu.SemaphoreType.DMA, pltpu.SemaphoreType.REGULAR
    in_vmem, in_hbm = pl.BlockSpec(memory_space=pltpu.VMEM), pl.BlockSpec(memory_space=pltpu.HBM)
    half = n_tok // 2
    results = pl.pallas_call(
        functools.partial(main_kernel, nz, ntp, rows, cols),
        out_shape=(pltpu.VMEM((cols, d), BF16), pltpu.VMEM((cols, d), BF16), pltpu.VMEM((q, d), BF16)),
        in_specs=[in_hbm] * 4,
        out_specs=(in_vmem, in_vmem, in_vmem),
        scratch_shapes=[
            pltpu.VMEM((n_tok, d), BF16),
            pltpu.VMEM((1, rows), F32),
            pltpu.VMEM((rows, cols), F32),
            pltpu.VMEM((rows, cols), F32),
            pltpu.VMEM((nz * size, LANES), BF16),
            pltpu.VMEM((nz * size, LANES), BF16),
            pltpu.VMEM((nz, n_tok, rows), BF16),
            pltpu.VMEM((n_tok, cols), F32),
            pltpu.VMEM((n_tok, cols), BF16),
            pltpu.VMEM((n_groups, half, wide), F32),
            pltpu.VMEM((n_groups, half, wide), BF16),
            pltpu.VMEM((n_groups, half, wide), BF16),
            pltpu.VMEM((n_groups, ny - 1, q, wide), BF16),
            pltpu.VMEM((n_groups, ny - 1, q, wide), BF16),
            pltpu.VMEM((n_groups, q, wide), F32),
            dma((4,)),
            dma((2, nz)),
            dma((2,)),
            dma((2, nz, 3)),
            dma,
            dma((2, nz)),
            dma((n_groups,)),
            dma((n_groups,)),
            dma((n_groups,)),
            dma((n_groups,)),
            regular,
            regular,
            regular,
            regular,
        ],
        compiler_params=pltpu.CompilerParams(
            collective_id=0, has_side_effects=True, vmem_limit_bytes=40 * 1024 * 1024
        ),
        name="gather_and_mix",
    )(*(pltpu.with_memory_space_constraint(v, pltpu.HBM) for v in (tokens, norm_gain.reshape(1, rows), up_master, down_master)))
    up_ready, down_ready, mixed_out = pl.pallas_call(
        final_kernel,
        out_shape=(pltpu.HBM((cols, d), BF16), pltpu.HBM((cols, d), BF16), pltpu.HBM((q, d), BF16)),
        in_specs=[in_vmem] * 3,
        out_specs=(in_hbm, in_hbm, in_hbm),
        scratch_shapes=[dma((2 * GROUPS + 1,))],
        compiler_params=pltpu.CompilerParams(vmem_limit_bytes=4 * 1024 * 1024),
        name="write_out",
    )(*results)
    return up_ready.T, down_ready.T, mixed_out


def solution(mesh):
    return jax.shard_map(
        functools.partial(per_device, mesh.shape["fs"], mesh.shape["tp"]),
        mesh=mesh,
        in_specs=(P(("grp", "fs"), None), P("fs"), P("fs", "tp"), P("fs", "tp")),
        out_specs=(P("grp", "tp"), P("grp", "tp"), P(("grp", "fs", "tp"), None)),
        check_vma=False,
    )
```
